32 devices in a mesh: ep: 4 (over y, x), tp: 8 (over z, core).
Axes of the slice: x: 2, y: 2, z: 4, core: 2. Of those that a mesh axis runs over, the one named last changes fastest.
Arguments:
- tokens: bfloat16 [128, 4096], P('ep'), may hold values from -6 to 6
- norm_gain: float32 [4096], replicated, may hold values from 0.1 to 1.9
- group_ids: int32 [128, 1], P('ep'), may hold values from 0 to 1; in each aligned block of 32 rows (0 to 31, 32 to 63, ...) at most 32 rows name the same one
- local_ids: int32 [128, 4], P('ep'), may hold values from 0 to 7, all different within a row
- group_gate: float32 [128], P('ep'), may hold values from 0.3 to 1
- expert_gate: float32 [128, 4], P('ep'), may hold values from 0.1 to 1
- lengths: int32 [32], P('ep'), may hold values from 1 to 4, 64 in all
- w_gate: bfloat16 [16, 1024, 4096], P('ep', 'tp'), may hold values from -0.09375 to 0.09375
- w_up: bfloat16 [16, 1024, 4096], P('ep', 'tp'), may hold values from -0.09375 to 0.09375
- w_down: bfloat16 [16, 1024, 4096], P('ep', None, 'tp'), may hold values from -0.1875 to 0.1875
Outputs:
- mixed: bfloat16 [128, 4096], P('ep', 'tp')
The draws below stay inside these ranges and needn't reach their ends.
Inputs may be any that keep to these rules, and one draw needn't show every extreme that they name: `group_ids`: among the 32 rows of one index of ep no group is named by more than 32 rows, and some index reaches 32. `local_ids`: each row names 4 different experts of its group. `lengths`: the first that many of a sequence's 4 positions are live.
All inputs are finite; a program needn't handle non-finite values. No bound on the sum of `lengths` on one device may be relied on, other than what follows from the above.
Results may differ from the reference program's by a relative error of at most 0.0065.
Values may be sent and summed in bfloat16 or wider, within the bound.
A program may use at most 64 MiB of HBM per device.

```python
import math
import jax
import jax.numpy as jnp
import numpy as np
from jax import lax

D = 4096
FF = 1024
EXP_PER_GROUP = 8
TOP_K = 4
STEP_TOK = 4
TOK_DEV = 32
SEQS = 32
TOKENS = 128
EXPERTS = 16
GROUPS = 2
CAP = 32


def levels(own_key, dims, shards, smallest, largest):
    def one(position, parts):
        steps = jax.random.uniform(jax.random.fold_in(jax.random.fold_in(own_key, 6), position), (parts,), jnp.float32, smallest / len(shards), largest / len(shards))
        return jnp.repeat(jnp.exp(steps), dims[position] // parts).reshape((-1,) + (1,) * (len(dims) - position - 1))

    factor_of = one(*shards[0])
    for cut in shards[1:]:
        factor_of = factor_of * one(*cut)
    return factor_of


def choose_distinct(key, rows, number_of, top, lift):
    ranking = jax.random.permutation(jax.random.fold_in(key, 1), number_of)
    pull = ranking
    for power in range(3):
        pull = pull * pull // number_of
    pull = pull * lift // number_of
    tickets = jax.random.randint(jax.random.fold_in(key, 2), (rows, number_of), 0, 4096) + pull
    sure = jax.random.permutation(jax.random.fold_in(key, 3), rows)[jnp.arange(number_of) % rows]
    tickets = jnp.where(jnp.arange(rows)[:, None] == sure[None, :], 1 << 14, tickets)
    merit = tickets * number_of + jnp.arange(number_of)
    return lax.top_k(merit.astype(jnp.int32), top)[1].astype(jnp.int32)


def length_profile(amount, total, bound, lean):
    weights = [(1 << 20) // math.isqrt(standing ** lean) + 1 for standing in range(2, amount + 1)]
    surplus, holding = total - bound - (amount - 1), [1] * (amount - 1)
    while surplus > 0:
        free = [i for i in range(amount - 1) if holding[i] < bound]
        mass, budget = sum([weights[i] for i in free]), surplus
        for i in free:
            more = min(bound - holding[i], max(1, budget * weights[i] // mass), surplus)
            holding[i] = holding[i] + more
            surplus = surplus - more
    return np.array([bound] + holding)


def uneven(own_key, count, total, limit, slope):
    if count == 2:
        one = jax.random.randint(own_key, (), max(1, total - limit), min(limit, total - 1) + 1)
        return jnp.stack([one, total - one])
    tallies = jnp.asarray(length_profile(count, total, limit, slope), jnp.int32)
    couples = (count - 1) // 2
    giver, taker = tallies[1:1 + 2 * couples:2], tallies[2:2 + 2 * couples:2]
    slack = jnp.minimum(giver - 1, limit - taker)
    moved = jax.random.randint(jax.random.fold_in(own_key, 1), (couples,), 0, 1 << 20) % (slack + 1)
    tallies = tallies.at[1:1 + 2 * couples:2].set(giver - moved).at[2:2 + 2 * couples:2].set(taker + moved)
    return tallies[jax.random.permutation(jax.random.fold_in(own_key, 2), count)]


def shared_out(key, own, number, rows, count, top, bound, slope):
    ranking = jax.random.permutation(key, count)
    packed, usual = shares(count, rows * top, bound, slope, True), shares(count, rows * top, bound, slope, False)
    places = jnp.arange(count)

    def named(sizes, offset_by):
        used = int((sizes > 0).sum())
        fixed = max(1, used // 4)
        shifted = fixed + (places - fixed + offset_by * (used - fixed)) % max(1, count - fixed)
        return jnp.zeros((count,), jnp.int32).at[ranking[jnp.where(places < fixed, places, shifted)]].set(jnp.asarray(sizes, jnp.int32))

    sizes = jnp.where(number % 4 == 0, named(packed, number // 4), named(usual, number - number // 4 - 1))
    mixed = jax.random.permutation(jax.random.fold_in(own, 3), count)
    donor, sink = mixed[0:count // 2 * 2:2], mixed[1:count // 2 * 2:2]
    margin = jnp.minimum(sizes[donor] - 1, bound - sizes[sink]) // 2
    margin = jnp.where((donor == ranking[0]) | (sink == ranking[0]) | (sizes[sink] == 0), 0, jnp.maximum(margin, 0))
    shifted = jax.random.randint(jax.random.fold_in(own, 4), (count // 2,), 0, 1 << 20) % (margin + 1)
    sizes = sizes.at[donor].add(-shifted).at[sink].add(shifted)
    labels = jnp.searchsorted(jnp.cumsum(sizes), jnp.arange(rows * top), side="right").astype(jnp.int32)
    listing = labels.reshape(top, rows).T
    listing = listing[jax.random.permutation(jax.random.fold_in(own, 1), rows)]
    offset_by = jax.random.randint(jax.random.fold_in(own, 2), (rows, 1), 0, top)
    return jnp.take_along_axis(listing, (jnp.arange(top)[None, :] + offset_by) % top, axis=1)


def shares(number_of, total, reach, skew, full):
    portions = [(1 << 20) // math.isqrt(rank ** skew) + 1 for rank in range(1, number_of + 1)]
    largest = reach if full else min(reach, max(-(-total // number_of), total * portions[0] // sum(portions)))
    least = 1 if total - largest >= number_of - 1 else 0
    given, rest = [largest] + [least] * (number_of - 1), total - largest - least * (number_of - 1)
    while rest > 0:
        movable = [i for i in range(1, number_of) if given[i] < largest] or [i for i in range(1, number_of) if given[i] < reach]
        whole, budget = sum([portions[i] for i in movable]), rest
        for i in movable:
            extra = min(reach - given[i], max(1, budget * portions[i] // whole), rest)
            given[i] = given[i] + extra
            rest = rest - extra
    return np.array(given)


def noise(rng, dims, deviation, reach, cuts=(), held_as=jnp.bfloat16):
    array = jax.random.normal(rng, dims, jnp.float32) * deviation
    if len(cuts) > 0:
        array = levels(rng, dims, cuts, -0.22, 0.18) * array
    return jnp.clip(array, min=-reach, max=reach).astype(held_as)


def setup_inputs(seed: int = 0) -> dict:
    keys = jax.random.split(jax.random.key(seed), 11)
    tokens = noise(keys[0], (TOKENS, D), 1.0, 6.0, ((0, 4),))
    norm_gain = jnp.clip(1.0 + 0.18 * jax.random.normal(keys[1], (D,), jnp.float32), 0.1, 1.9)
    group_ids_keys = jax.random.split(jax.random.fold_in(keys[2], 1), TOKENS // TOK_DEV)
    group_ids_turns = jax.random.permutation(jax.random.fold_in(keys[2], 3), TOKENS // TOK_DEV)
    group_ids = jax.vmap(lambda own, number: shared_out(jax.random.fold_in(keys[2], 2), own, number, TOK_DEV, GROUPS, 1, CAP, 2))(group_ids_keys, group_ids_turns).reshape((TOKENS, 1))
    local_ids = choose_distinct(keys[3], TOKENS, EXP_PER_GROUP, TOP_K, 8192)
    group_gate = jnp.clip(jnp.exp(math.log(1.0) - 1.2039728 * jax.random.uniform(keys[4], (TOKENS,), jnp.float32) ** levels(keys[4], (TOKENS,), ((0, 4),), -0.2, 0.2)), 0.3, 1.0)
    expert_gate = jnp.clip(0.1 + 0.9 * jax.random.uniform(keys[5], (TOKENS, TOP_K), jnp.float32) ** levels(keys[5], (TOKENS, TOP_K), ((0, 4),), -0.2, 0.2), 0.1, 1.0)
    lengths = uneven(keys[6], SEQS, SEQS * STEP_TOK // 2, STEP_TOK, 2).astype(jnp.int32)
    w_gate = noise(keys[7], (EXPERTS, FF, D), D ** -0.5, 0.09375, ((0, 4), (1, 8)))
    w_up = noise(keys[8], (EXPERTS, FF, D), D ** -0.5, 0.09375, ((0, 4), (1, 8)))
    w_down = noise(keys[9], (EXPERTS, FF, D), FF ** -0.5, 0.1875, ((0, 4), (2, 8)))
    return {"tokens": tokens, "norm_gain": norm_gain, "group_ids": group_ids, "local_ids": local_ids, "group_gate": group_gate, "expert_gate": expert_gate, "lengths": lengths, "w_gate": w_gate, "w_up": w_up, "w_down": w_down}


def reference(tokens, norm_gain, group_ids, local_ids, group_gate, expert_gate, lengths, w_gate, w_up, w_down):
    values = tokens.astype(jnp.float32)
    scale = lax.rsqrt(lax.optimization_barrier(jnp.mean(values * values, axis=1, keepdims=True)) + 1e-06)
    normed = (values * scale * norm_gain).astype(jnp.bfloat16)
    places = jnp.arange(TOKENS, dtype=jnp.int32)
    live = (places % STEP_TOK < lengths[places // STEP_TOK]).astype(jnp.float32)
    chosen = group_ids * EXP_PER_GROUP + local_ids
    weights = expert_gate * (group_gate * live)[:, None]

    def add_expert(index, total):
        share = lax.optimization_barrier(jnp.sum(jnp.where(chosen == index, weights, jnp.zeros_like(weights)), axis=1))
        gate_part = jnp.dot(normed, w_gate[index].T, preferred_element_type=jnp.float32)
        up_part = jnp.dot(normed, w_up[index].T, preferred_element_type=jnp.float32)
        hidden = (jax.nn.silu(gate_part) * up_part).astype(jnp.bfloat16)
        result = jnp.dot(hidden, w_down[index], preferred_element_type=jnp.float32)
        return total + share[:, None] * result
    total = lax.fori_loop(0, EXPERTS, add_expert, jnp.zeros((TOKENS, D), jnp.float32))
    return total.astype(jnp.bfloat16)
```

```python
import functools

import jax
import jax.numpy as jnp
from jax import lax
from jax.experimental import pallas as pl
from jax.experimental.pallas import tpu as pltpu
from jax.sharding import PartitionSpec as P

EXP_PER_GROUP = 8
STEP_TOK = 4
CORES = 2
CHUNKS = 4
MESH = pl.DeviceIdType.MESH
F32 = jnp.float32
BF16 = jnp.bfloat16


def token_table(group_ids, local_ids, group_gate, expert_gate, lengths, ep_size, exp_dev):
    top_k, tok_rows = local_ids.shape
    seqs = lengths.shape[1]
    rows = table_rows(exp_dev)
    here = lax.broadcasted_iota(jnp.int32, (seqs, seqs), 0) == lax.broadcasted_iota(jnp.int32, (seqs, seqs), 1)
    column = jnp.sum(jnp.where(here, lengths.astype(F32), 0.0), axis=1, keepdims=True)
    place = lax.broadcasted_iota(jnp.int32, (seqs, tok_rows), 1)
    first = lax.broadcasted_iota(jnp.int32, (seqs, tok_rows), 0) * STEP_TOK
    hits = (place >= first) & (place < first + STEP_TOK) & ((place - first).astype(F32) < column)
    live = jnp.sum(jnp.where(hits, 1.0, 0.0), axis=0, keepdims=True)
    weights = expert_gate * (group_gate * live)
    chosen = group_ids * EXP_PER_GROUP + local_ids
    parts = []
    for owner in range(ep_size):
        row = lax.broadcasted_iota(jnp.int32, (rows, tok_rows), 0)
        part = jnp.where(row == exp_dev, live, 0.0)
        expert = jnp.where(row < exp_dev, owner * exp_dev + row, -1)
        for c in range(top_k):
            part = part + jnp.where(expert == chosen[c:c + 1], weights[c:c + 1], 0.0)
        parts.append(part)
    return parts


def table_rows(exp_dev):
    return -(-(exp_dev + 1) // 8) * 8


def kernel(
    ep_size, tp_size,
    tokens_hbm, gain_ref, group_ref, local_ref, group_gate_ref, expert_gate_ref, lengths_ref, wg_hbm, wu_hbm, wd_hbm,
    out_ref,
    tok, x_all, table_ref, meta, wgu, wd, acc, hid, y_send, y_recv,
    tok_sem, wg_sem, wu_sem, wd_sem,
    meta_send, meta_recv, row_send, row_recv, rowf_send, rowf_recv,
    hid_send, hid_recv, hidp_send, hidp_recv, back_send, back_recv,
):
    exp_dev, part, depth = wg_hbm.shape
    tok_rows = tok.shape[0]
    half = tok_rows // CORES
    n_tok = ep_size * tok_rows
    n_slot = n_tok // 2
    step = depth // CHUNKS
    chips = tp_size // CORES
    ep = lax.axis_index("ep")
    tp = lax.axis_index("tp")
    core = lax.rem(tp, CORES)
    chip = tp // CORES
    partner = chip * CORES + (1 - core)

    def remote(src, dst, send, recv, to_ep, to_tp):
        return pltpu.make_async_remote_copy(
            src_ref=src, dst_ref=dst, send_sem=send, recv_sem=recv,
            device_id=(to_ep, to_tp), device_id_type=MESH,
        )

    def ep_at(off):
        return lax.rem(ep + off + ep_size, ep_size)

    def tp_at(off):
        return lax.rem(chip + off + chips, chips) * CORES + core

    tok_copy = pltpu.make_async_copy(tokens_hbm, tok, tok_sem)
    tok_copy.start()
    wg_copies, wu_copies, wd_copies = [], [], []
    for e in range(exp_dev):
        wg_copies.append(pltpu.make_async_copy(wg_hbm.at[e], wgu.at[e, pl.ds(0, part)], wg_sem.at[e]))
        wu_copies.append(pltpu.make_async_copy(wu_hbm.at[e], wgu.at[e, pl.ds(part, part)], wu_sem.at[e]))
        wd_copies.append(pltpu.make_async_copy(wd_hbm.at[e], wd.at[e], wd_sem.at[e]))
    for copy in wg_copies + wu_copies + wd_copies:
        copy.start()

    barrier = pltpu.get_barrier_semaphore()
    for off in range(1, ep_size):
        pl.semaphore_signal(barrier, inc=1, device_id=(ep_at(off), tp), device_id_type=MESH)
    for off in range(1, chips):
        pl.semaphore_signal(barrier, inc=1, device_id=(ep, tp_at(off)), device_id_type=MESH)
    pl.semaphore_signal(barrier, inc=1, device_id=(ep, partner), device_id_type=MESH)

    tables = token_table(
        group_ref[...], local_ref[...], group_gate_ref[...], expert_gate_ref[...], lengths_ref[...], ep_size, exp_dev
    )
    for i in range(ep_size):
        table_ref[i] = tables[i]
    tok_copy.wait()
    values = tok[...].astype(F32)
    scale = lax.rsqrt(jnp.mean(values * values, axis=1, keepdims=True) + 1e-06)
    x_all[ep] = (values * scale * gain_ref[...]).astype(BF16)
    meta[ep] = table_ref[ep]

    pl.semaphore_wait(barrier, ep_size - 1 + chips - 1 + 1)

    pending = []
    for off in range(1, ep_size):
        copy = remote(table_ref.at[ep_at(off)], meta.at[ep], meta_send.at[off], meta_recv.at[off], ep_at(off), tp)
        copy.start()
        pending.append(copy)

    def rows_of(owner, which, q):
        return x_all.at[owner, pl.ds(pl.multiple_of(which * half, half), half), pl.ds(q * step, step)]

    row_copies = {}
    for q in range(CHUNKS):
        for off in range(1, ep_size):
            block = rows_of(ep, core, q)
            copy = remote(block, block, row_send.at[q, off], row_recv.at[q, off], ep_at(off), tp)
            copy.start()
            row_copies[q, off] = copy
            pending.append(copy)

    for off in range(1, ep_size):
        remote(table_ref.at[ep], meta.at[ep_at(-off)], meta_send.at[off], meta_recv.at[off], ep, tp).wait_recv()
    table = jnp.concatenate([meta[i] for i in range(ep_size)], axis=1)
    live = table[exp_dev:exp_dev + 1, :]
    before = (
        lax.broadcasted_iota(jnp.int32, (n_tok, n_tok), 0) < lax.broadcasted_iota(jnp.int32, (n_tok, n_tok), 1)
    ).astype(F32)
    rank = jnp.dot(
        jnp.broadcast_to(live, (8, n_tok)).astype(BF16), before.astype(BF16), preferred_element_type=F32
    )[0:1, :]
    slot = lax.broadcasted_iota(jnp.int32, (n_tok, n_tok), 0).astype(F32)
    place = jnp.where((slot == rank) & (live > 0.5), 1.0, 0.0)
    pick = place[:n_slot, :]
    spread = jnp.transpose(place)[:, :n_slot].astype(BF16)
    pick16 = pick.astype(BF16)
    gates = [jnp.sum(pick * table[e:e + 1, :], axis=1, keepdims=True) for e in range(exp_dev)]

    def send_hidden(e):
        both = acc[e]
        gate, up = both[:, :part], both[:, part:]
        hid[e, tp] = (jax.nn.silu(gate) * up).astype(BF16)
        block = hid.at[e, tp]
        for off in range(1, chips):
            copy = remote(block, block, hid_send.at[e, off], hid_recv.at[e, off], ep, tp_at(off))
            copy.start()
            pending.append(copy)
        copy = remote(block, block, hidp_send.at[e, 0], hidp_recv.at[e, 0], ep, partner)
        copy.start()
        pending.append(copy)

    for q in range(CHUNKS + 1):
        if q < CHUNKS:
            for off in range(1, ep_size):
                block = rows_of(ep_at(-off), core, q)
                row_copies[q, off].wait_recv()
                copy = remote(block, block, rowf_send.at[q, off], rowf_recv.at[q, off], ep, partner)
                copy.start()
                pending.append(copy)
                row_copies[q, off] = copy
        if q > 0:
            k = q - 1
            for off in range(1, ep_size):
                row_copies[k, off].wait_recv()
            chunk = jnp.concatenate([x_all[i, :, pl.ds(k * step, step)] for i in range(ep_size)], axis=0)
            rows = jnp.dot(pick16, chunk, preferred_element_type=F32).astype(BF16)
            for e in range(exp_dev):
                if k == 0:
                    wg_copies[e].wait()
                    wu_copies[e].wait()
                new = lax.dot_general(
                    rows, wgu[e, :, pl.ds(k * step, step)], (((1,), (1,)), ((), ())), preferred_element_type=F32
                )
                acc[e] = new if k == 0 else acc[e] + new
                if k == CHUNKS - 1:
                    send_hidden(e)

    hid_copies = {}
    total = None
    for e in range(exp_dev + 1):
        if e < exp_dev:
            for off in range(1, chips):
                block = hid.at[e, tp_at(-off)]
                remote(block, block, hid_send.at[e, off], hid_recv.at[e, off], ep, tp_at(off)).wait_recv()
                copy = remote(block, block, hidp_send.at[e, off], hidp_recv.at[e, off], ep, partner)
                copy.start()
                pending.append(copy)
                hid_copies[e, off] = copy
        if e > 0:
            k = e - 1
            block = hid.at[k, tp]
            remote(block, block, hidp_send.at[k, 0], hidp_recv.at[k, 0], ep, partner).wait_recv()
            for off in range(1, chips):
                hid_copies[k, off].wait_recv()
            wd_copies[k].wait()
            hidden = jnp.concatenate([hid[k, j] for j in range(tp_size)], axis=1)
            term = gates[k] * jnp.dot(hidden, wd[k], preferred_element_type=F32)
            total = term if total is None else total + term

    back = jnp.dot(spread, total.astype(BF16), preferred_element_type=F32).astype(BF16)
    for i in range(ep_size):
        y_send[i] = back[i * tok_rows:(i + 1) * tok_rows]
    back_copies = []
    for off in range(1, ep_size):
        copy = remote(y_send.at[ep_at(off)], y_recv.at[off], back_send.at[off], back_recv.at[off], ep_at(off), tp)
        copy.start()
        back_copies.append(copy)
    mixed = y_send[ep].astype(F32)
    for off in range(1, ep_size):
        back_copies[off - 1].wait_recv()
        mixed = mixed + y_recv[off].astype(F32)
    out_ref[...] = mixed.astype(BF16)
    for copy in pending + back_copies:
        copy.wait_send()


def local(
    ep_size, tp_size,
    tokens, norm_gain, group_ids, local_ids, group_gate, expert_gate, lengths, w_gate, w_up, w_down
):
    tok_rows, depth = tokens.shape
    exp_dev, part, _ = w_gate.shape
    _, hidden_all, width = w_down.shape
    chips = tp_size // CORES
    n_slot = ep_size * tok_rows // 2
    rows = table_rows(exp_dev)
    anywhere = pl.BlockSpec(memory_space=pl.ANY)
    vmem = pl.BlockSpec(memory_space=pltpu.VMEM)
    dma = pltpu.SemaphoreType.DMA
    return pl.pallas_call(
        functools.partial(kernel, ep_size, tp_size),
        out_shape=jax.ShapeDtypeStruct((tok_rows, width), BF16),
        in_specs=[anywhere, vmem, vmem, vmem, vmem, vmem, vmem, anywhere, anywhere, anywhere],
        out_specs=vmem,
        scratch_shapes=[
            pltpu.VMEM((tok_rows, depth), BF16),
            pltpu.VMEM((ep_size, tok_rows, depth), BF16),
            pltpu.VMEM((ep_size, rows, tok_rows), F32),
            pltpu.VMEM((ep_size, rows, tok_rows), F32),
            pltpu.VMEM((exp_dev, 2 * part, depth), BF16),
            pltpu.VMEM((exp_dev, hidden_all, width), BF16),
            pltpu.VMEM((exp_dev, n_slot, 2 * part), F32),
            pltpu.VMEM((exp_dev, tp_size, n_slot, part), BF16),
            pltpu.VMEM((ep_size, tok_rows, width), BF16),
            pltpu.VMEM((ep_size, tok_rows, width), BF16),
            dma, dma((exp_dev,)), dma((exp_dev,)), dma((exp_dev,)),
            dma((ep_size,)), dma((ep_size,)),
            dma((CHUNKS, ep_size)), dma((CHUNKS, ep_size)), dma((CHUNKS, ep_size)), dma((CHUNKS, ep_size)),
            dma((exp_dev, chips)), dma((exp_dev, chips)), dma((exp_dev, chips)), dma((exp_dev, chips)),
            dma((ep_size,)), dma((ep_size,)),
        ],
        compiler_params=pltpu.CompilerParams(collective_id=0, has_side_effects=True),
    )(
        tokens, norm_gain.reshape(1, depth), group_ids.T, local_ids.T, group_gate.reshape(1, tok_rows),
        expert_gate.T, lengths.reshape(1, -1), w_gate, w_up, w_down,
    )


def solution(mesh):
    in_specs = (
        P("ep", None),
        P(),
        P("ep", None),
        P("ep", None),
        P("ep"),
        P("ep", None),
        P("ep"),
        P("ep", "tp", None),
        P("ep", "tp", None),
        P("ep", None, "tp"),
    )
    body = functools.partial(local, mesh.shape["ep"], mesh.shape["tp"])
    return jax.shard_map(body, mesh=mesh, in_specs=in_specs, out_specs=P("ep", "tp"), check_vma=False)
```

```python
import functools

import jax
import jax.numpy as jnp
from jax import lax
from jax.experimental import pallas as pl
from jax.experimental.pallas import tpu as pltpu
from jax.sharding import PartitionSpec as P

EXP_PER_GROUP = 8
STEP_TOK = 4
CORES = 2
CHUNKS = 4
MESH = pl.DeviceIdType.MESH
F32 = jnp.float32
BF16 = jnp.bfloat16


def token_table(group_ids, local_ids, group_gate, expert_gate, lengths, ep_size, exp_dev):
    top_k, tok_rows = local_ids.shape
    seqs = lengths.shape[1]
    rows = table_rows(exp_dev)
    here = lax.broadcasted_iota(jnp.int32, (seqs, seqs), 0) == lax.broadcasted_iota(jnp.int32, (seqs, seqs), 1)
    column = jnp.sum(jnp.where(here, lengths.astype(F32), 0.0), axis=1, keepdims=True)
    place = lax.broadcasted_iota(jnp.int32, (seqs, tok_rows), 1)
    first = lax.broadcasted_iota(jnp.int32, (seqs, tok_rows), 0) * STEP_TOK
    hits = (place >= first) & (place < first + STEP_TOK) & ((place - first).astype(F32) < column)
    live = jnp.sum(jnp.where(hits, 1.0, 0.0), axis=0, keepdims=True)
    weights = expert_gate * (group_gate * live)
    chosen = group_ids * EXP_PER_GROUP + local_ids
    parts = []
    for owner in range(ep_size):
        row = lax.broadcasted_iota(jnp.int32, (rows, tok_rows), 0)
        part = jnp.where(row == exp_dev, live, 0.0)
        expert = jnp.where(row < exp_dev, owner * exp_dev + row, -1)
        for c in range(top_k):
            part = part + jnp.where(expert == chosen[c:c + 1], weights[c:c + 1], 0.0)
        parts.append(part)
    return parts


def table_rows(exp_dev):
    return -(-(exp_dev + 1) // 8) * 8


def kernel(
    ep_size, tp_size,
    tokens_hbm, gain_hbm, group_hbm, local_hbm, group_gate_hbm, expert_gate_hbm, lengths_hbm, wg_hbm, wu_hbm, wd_hbm,
    out_ref,
    tok, gain_ref, group_ref, local_ref, group_gate_ref, expert_gate_ref, lengths_ref, x_all, table_ref, meta, wgu, wd, acc, hid, y_send, y_recv,
    tok_sem, small_sem, wg_sem, wu_sem, wd_sem,
    meta_send, meta_recv, row_send, row_recv, rowf_send, rowf_recv,
    hid_send, hid_recv, hidp_send, hidp_recv, back_send, back_recv,
):
    exp_dev, part, depth = wg_hbm.shape
    tok_rows = tok.shape[0]
    half = tok_rows // CORES
    n_tok = ep_size * tok_rows
    n_slot = n_tok // 2
    step = depth // CHUNKS
    chips = tp_size // CORES
    ep = lax.axis_index("ep")
    tp = lax.axis_index("tp")
    core = lax.rem(tp, CORES)
    chip = tp // CORES
    partner = chip * CORES + (1 - core)

    def remote(src, dst, send, recv, to_ep, to_tp):
        return pltpu.make_async_remote_copy(
            src_ref=src, dst_ref=dst, send_sem=send, recv_sem=recv,
            device_id=(to_ep, to_tp), device_id_type=MESH,
        )

    def ep_at(off):
        return lax.rem(ep + off + ep_size, ep_size)

    def tp_at(off):
        return lax.rem(chip + off + chips, chips) * CORES + core

    tok_copy = pltpu.make_async_copy(tokens_hbm, tok, tok_sem)
    tok_copy.start()
    small = [
        pltpu.make_async_copy(src, dst, small_sem.at[n])
        for n, (src, dst) in enumerate([
            (group_hbm, group_ref), (local_hbm, local_ref), (group_gate_hbm, group_gate_ref),
            (expert_gate_hbm, expert_gate_ref), (lengths_hbm, lengths_ref), (gain_hbm, gain_ref),
        ])
    ]
    for copy in small:
        copy.start()
    barrier = pltpu.get_barrier_semaphore()
    for off in range(1, ep_size):
        pl.semaphore_signal(barrier, inc=1, device_id=(ep_at(off), tp), device_id_type=MESH)
    for off in range(1, chips):
        pl.semaphore_signal(barrier, inc=1, device_id=(ep, tp_at(off)), device_id_type=MESH)
    pl.semaphore_signal(barrier, inc=1, device_id=(ep, partner), device_id_type=MESH)

    wg_copies, wu_copies, wd_copies = [], [], []
    for e in range(exp_dev):
        wg_copies.append(pltpu.make_async_copy(wg_hbm.at[e], wgu.at[e, pl.ds(0, part)], wg_sem.at[e]))
        wu_copies.append(pltpu.make_async_copy(wu_hbm.at[e], wgu.at[e, pl.ds(part, part)], wu_sem.at[e]))
        wd_copies.append(pltpu.make_async_copy(wd_hbm.at[e], wd.at[e], wd_sem.at[e]))
    for copy in small:
        copy.wait()
    tables = token_table(
        group_ref[...], local_ref[...], group_gate_ref[...], expert_gate_ref[...], lengths_ref[...], ep_size, exp_dev
    )
    for i in range(ep_size):
        table_ref[i] = tables[i]
    tok_copy.wait()
    for copy in wg_copies + wu_copies + wd_copies:
        copy.start()
    values = tok[...].astype(F32)
    scale = lax.rsqrt(jnp.mean(values * values, axis=1, keepdims=True) + 1e-06)
    x_all[ep] = (values * scale * gain_ref[...]).astype(BF16)
    meta[ep] = table_ref[ep]

    pl.semaphore_wait(barrier, ep_size - 1 + chips - 1 + 1)

    pending = []
    for off in range(1, ep_size):
        copy = remote(table_ref.at[ep_at(off)], meta.at[ep], meta_send.at[off], meta_recv.at[off], ep_at(off), tp)
        copy.start()
        pending.append(copy)

    def rows_of(owner, which, q):
        return x_all.at[owner, pl.ds(pl.multiple_of(which * half, half), half), pl.ds(q * step, step)]

    row_copies = {}
    for q in range(CHUNKS):
        for off in range(1, ep_size):
            block = rows_of(ep, core, q)
            copy = remote(block, block, row_send.at[q, off], row_recv.at[q, off], ep_at(off), tp)
            copy.start()
            row_copies[q, off] = copy
            pending.append(copy)

    for off in range(1, ep_size):
        remote(table_ref.at[ep], meta.at[ep_at(-off)], meta_send.at[off], meta_recv.at[off], ep, tp).wait_recv()
    table = jnp.concatenate([meta[i] for i in range(ep_size)], axis=1)
    live = table[exp_dev:exp_dev + 1, :]
    before = (
        lax.broadcasted_iota(jnp.int32, (n_tok, n_tok), 0) < lax.broadcasted_iota(jnp.int32, (n_tok, n_tok), 1)
    ).astype(F32)
    rank = jnp.dot(
        jnp.broadcast_to(live, (8, n_tok)).astype(BF16), before.astype(BF16), preferred_element_type=F32
    )[0:1, :]
    slot = lax.broadcasted_iota(jnp.int32, (n_tok, n_tok), 0).astype(F32)
    place = jnp.where((slot == rank) & (live > 0.5), 1.0, 0.0)
    pick = place[:n_slot, :]
    spread = jnp.transpose(place)[:, :n_slot].astype(BF16)
    pick16 = pick.astype(BF16)
    gates = [jnp.sum(pick * table[e:e + 1, :], axis=1, keepdims=True) for e in range(exp_dev)]

    def send_hidden(e):
        both = acc[e]
        gate, up = both[:, :part], both[:, part:]
        hid[e, tp] = (jax.nn.silu(gate) * up).astype(BF16)
        block = hid.at[e, tp]
        for off in range(1, chips):
            copy = remote(block, block, hid_send.at[e, off], hid_recv.at[e, off], ep, tp_at(off))
            copy.start()
            pending.append(copy)
        copy = remote(block, block, hidp_send.at[e, 0], hidp_recv.at[e, 0], ep, partner)
        copy.start()
        pending.append(copy)

    for q in range(CHUNKS + 1):
        if q < CHUNKS:
            for off in range(1, ep_size):
                block = rows_of(ep_at(-off), core, q)
                row_copies[q, off].wait_recv()
                copy = remote(block, block, rowf_send.at[q, off], rowf_recv.at[q, off], ep, partner)
                copy.start()
                pending.append(copy)
                row_copies[q, off] = copy
        if q > 0:
            k = q - 1
            for off in range(1, ep_size):
                row_copies[k, off].wait_recv()
            chunk = jnp.concatenate([x_all[i, :, pl.ds(k * step, step)] for i in range(ep_size)], axis=0)
            rows = jnp.dot(pick16, chunk, preferred_element_type=F32).astype(BF16)
            for e in range(exp_dev):
                if k == 0:
                    wg_copies[e].wait()
                    wu_copies[e].wait()
                new = lax.dot_general(
                    rows, wgu[e, :, pl.ds(k * step, step)], (((1,), (1,)), ((), ())), preferred_element_type=F32
                )
                acc[e] = new if k == 0 else acc[e] + new
                if k == CHUNKS - 1:
                    send_hidden(e)

    hid_copies = {}
    total = None
    for e in range(exp_dev + 1):
        if e < exp_dev:
            for off in range(1, chips):
                block = hid.at[e, tp_at(-off)]
                remote(block, block, hid_send.at[e, off], hid_recv.at[e, off], ep, tp_at(off)).wait_recv()
                copy = remote(block, block, hidp_send.at[e, off], hidp_recv.at[e, off], ep, partner)
                copy.start()
                pending.append(copy)
                hid_copies[e, off] = copy
        if e > 0:
            k = e - 1
            block = hid.at[k, tp]
            remote(block, block, hidp_send.at[k, 0], hidp_recv.at[k, 0], ep, partner).wait_recv()
            for off in range(1, chips):
                hid_copies[k, off].wait_recv()
            wd_copies[k].wait()
            hidden = jnp.concatenate([hid[k, j] for j in range(tp_size)], axis=1)
            term = gates[k] * jnp.dot(hidden, wd[k], preferred_element_type=F32)
            total = term if total is None else total + term

    back = jnp.dot(spread, total.astype(BF16), preferred_element_type=F32).astype(BF16)
    for i in range(ep_size):
        y_send[i] = back[i * tok_rows:(i + 1) * tok_rows]
    back_copies = []
    for off in range(1, ep_size):
        copy = remote(y_send.at[ep_at(off)], y_recv.at[off], back_send.at[off], back_recv.at[off], ep_at(off), tp)
        copy.start()
        back_copies.append(copy)
    mixed = y_send[ep].astype(F32)
    for off in range(1, ep_size):
        back_copies[off - 1].wait_recv()
        mixed = mixed + y_recv[off].astype(F32)
    out_ref[...] = mixed.astype(BF16)
    for copy in pending + back_copies:
        copy.wait_send()


def local(
    ep_size, tp_size,
    tokens, norm_gain, group_ids, local_ids, group_gate, expert_gate, lengths, w_gate, w_up, w_down
):
    tok_rows, depth = tokens.shape
    exp_dev, part, _ = w_gate.shape
    _, hidden_all, width = w_down.shape
    chips = tp_size // CORES
    n_slot = ep_size * tok_rows // 2
    rows = table_rows(exp_dev)
    anywhere = pl.BlockSpec(memory_space=pl.ANY)
    vmem = pl.BlockSpec(memory_space=pltpu.VMEM)
    dma = pltpu.SemaphoreType.DMA
    return pl.pallas_call(
        functools.partial(kernel, ep_size, tp_size),
        out_shape=jax.ShapeDtypeStruct((tok_rows, width), BF16),
        in_specs=[anywhere] * 10,
        out_specs=vmem,
        scratch_shapes=[
            pltpu.VMEM((tok_rows, depth), BF16),
            pltpu.VMEM((1, depth), F32),
            pltpu.VMEM((1, tok_rows), jnp.int32),
            pltpu.VMEM((local_ids.shape[1], tok_rows), jnp.int32),
            pltpu.VMEM((1, tok_rows), F32),
            pltpu.VMEM((local_ids.shape[1], tok_rows), F32),
            pltpu.VMEM((1, lengths.shape[0]), jnp.int32),
            pltpu.VMEM((ep_size, tok_rows, depth), BF16),
            pltpu.VMEM((ep_size, rows, tok_rows), F32),
            pltpu.VMEM((ep_size, rows, tok_rows), F32),
            pltpu.VMEM((exp_dev, 2 * part, depth), BF16),
            pltpu.VMEM((exp_dev, hidden_all, width), BF16),
            pltpu.VMEM((exp_dev, n_slot, 2 * part), F32),
            pltpu.VMEM((exp_dev, tp_size, n_slot, part), BF16),
            pltpu.VMEM((ep_size, tok_rows, width), BF16),
            pltpu.VMEM((ep_size, tok_rows, width), BF16),
            dma, dma((6,)), dma((exp_dev,)), dma((exp_dev,)), dma((exp_dev,)),
            dma((ep_size,)), dma((ep_size,)),
            dma((CHUNKS, ep_size)), dma((CHUNKS, ep_size)), dma((CHUNKS, ep_size)), dma((CHUNKS, ep_size)),
            dma((exp_dev, chips)), dma((exp_dev, chips)), dma((exp_dev, chips)), dma((exp_dev, chips)),
            dma((ep_size,)), dma((ep_size,)),
        ],
        compiler_params=pltpu.CompilerParams(collective_id=0, has_side_effects=True),
    )(
        tokens, norm_gain.reshape(1, depth), group_ids.T, local_ids.T, group_gate.reshape(1, tok_rows),
        expert_gate.T, lengths.reshape(1, -1), w_gate, w_up, w_down,
    )


def solution(mesh):
    in_specs = (
        P("ep", None),
        P(),
        P("ep", None),
        P("ep", None),
        P("ep"),
        P("ep", None),
        P("ep"),
        P("ep", "tp", None),
        P("ep", "tp", None),
        P("ep", None, "tp"),
    )
    body = functools.partial(local, mesh.shape["ep"], mesh.shape["tp"])
    return jax.shard_map(body, mesh=mesh, in_specs=in_specs, out_specs=P("ep", "tp"), check_vma=False)
```
